256 devices in a mesh: grp: 2 (over y), sp: 16 (over z), tp: 8 (over x, core).
Axes of the slice: x: 4, y: 2, z: 16, core: 2. Of those that a mesh axis runs over, the one named last changes fastest.
The devices are a block of a 4x16x16 slice.
Arguments:
- tokens: bfloat16 [16384, 2, 2048], P(('grp', 'sp', 'tp')), parts along dimension 0, may hold values from -64 to 64
- w_query: bfloat16 [2048, 2048], P(None, 'tp'), may hold values from -0.21875 to 0.21875
- w_key: bfloat16 [2048, 2048], P(None, 'tp'), may hold values from -0.125 to 0.125
- w_value: bfloat16 [2048, 2048], P(None, 'tp'), may hold values from -0.125 to 0.125
- w_out: bfloat16 [2048, 2048], P('tp'), may hold values from -0.125 to 0.125
- head_lambda: float32 [16], P('tp'), may hold values from 0.3 to 0.8
- sub_gain: float32 [128], replicated, may hold values from 0.1 to 1.9
Outputs:
- mixed: bfloat16 [16384, 2, 2048], P(('grp', 'sp', 'tp')), parts along dimension 0
The draws below stay inside these ranges and needn't reach their ends.
There are 2 independent parts, one for each index of `grp`. The reference program is written for one: setup_inputs(seed, part) draws one part's arguments, and reference() takes and returns one part's arrays. A program takes and returns all parts, laid end to end along the dimension named above; an argument that names none is the same for every part. Nothing has to cross between parts.
All inputs are finite; a program needn't handle non-finite values.
Results may differ from the reference program's by a relative error of at most 0.015.
The reference program's roundings to bfloat16 on the way count: a program that leaves them out, or rounds other values in their place, can miss the bound.
Values may be sent and summed in bfloat16 or wider, within the bound.
A program may use at most 128 MiB of HBM per device.

```python
import math
import jax
import jax.numpy as jnp
from jax import lax

D = 2048
HEAD = 64
SPAN = 64
SEQS = 2
TOK_DEV = 512
HEADS = 16
LENGTH = 8192
N_TP = 8


def draw_tokens(key, part):
    key_base, key_shift = jax.random.split(jax.random.fold_in(key, 11), 2)
    base = jax.random.normal(key_base, (LENGTH, SEQS, D), jnp.float32)
    shifts = 0.6 * jax.random.normal(key_shift, (LENGTH // TOK_DEV, SEQS, D), jnp.float32)
    base = base + jnp.repeat(shifts, TOK_DEV, axis=0)
    return jnp.clip(base, -64.0, 64.0).astype(jnp.bfloat16)


def steps_of(own_key, dims, cuts, smallest, high):
    loudness, own = 1.0, jax.random.fold_in(own_key, 6)
    for position, blocks in cuts:
        heights = jnp.exp(jax.random.uniform(jax.random.fold_in(own, position), (blocks,), jnp.float32, smallest / len(cuts), high / len(cuts)))
        loudness = loudness * jnp.repeat(heights, dims[position] // blocks).reshape([-1 if axis == position else 1 for axis in range(len(dims))])
    return loudness


def bell_draw(own_key, extent, spread, bound, shards=(), held_as=jnp.bfloat16):
    result = spread * jax.random.normal(own_key, extent, jnp.float32)
    if shards:
        result = result * steps_of(own_key, extent, shards, -0.22, 0.18)
    return jnp.clip(result, -bound, bound).astype(held_as)


def setup_inputs(seed: int = 0, part: int = 0) -> dict:
    keys = jax.random.split(jax.random.key(seed), 8)
    part_splits = jax.random.split(jax.random.fold_in(keys[7], part), 8)
    return {
        "tokens": draw_tokens(jax.random.fold_in(jax.random.fold_in(keys[7], part), 71), part),
        "w_query": bell_draw(keys[1], (D, D), (D // 3) ** -0.5, 0.21875, ((1, 8),)),
        "w_key": bell_draw(keys[2], (D, D), D ** -0.5, 0.125, ((1, 8),)),
        "w_value": bell_draw(keys[3], (D, D), D ** -0.5, 0.125, ((1, 8),)),
        "w_out": bell_draw(keys[4], (D, D), D ** -0.5, 0.125, ((0, 8),)),
        "head_lambda": jnp.clip(0.3 + 0.5 * jax.random.uniform(keys[5], (HEADS,), jnp.float32) ** steps_of(keys[5], (HEADS,), ((0, 8),), -0.2, 0.2), 0.3, 0.8),
        "sub_gain": jnp.clip(1.0 + 0.18 * jax.random.normal(keys[6], (2 * HEAD,), jnp.float32), 0.1, 1.9),
    }


def one_sequence(seq_tokens, w_query, w_key, w_value, w_out, head_lambda, sub_gain):
    total_rows = seq_tokens.shape[0]
    head_count = head_lambda.shape[0]
    value_dim = 2 * HEAD
    queries = jnp.dot(seq_tokens, w_query, preferred_element_type=jnp.float32).astype(jnp.bfloat16)
    queries = queries.reshape(total_rows, head_count, 2, HEAD).transpose(1, 0, 2, 3)
    keys_all = jnp.dot(seq_tokens, w_key, preferred_element_type=jnp.float32).astype(jnp.bfloat16)
    keys_all = keys_all.reshape(total_rows, head_count, 2, HEAD).transpose(1, 0, 2, 3)
    values = jnp.dot(seq_tokens, w_value, preferred_element_type=jnp.float32).astype(jnp.bfloat16)
    values = values.reshape(total_rows, head_count, value_dim).transpose(1, 0, 2)
    blk_len = math.gcd(total_rows, 512)
    blk_count = total_rows // blk_len
    positions = jnp.arange(total_rows, dtype=jnp.int32)

    def one_head(head_args):
        head_q, head_k, head_v, head_lam = head_args
        key_f = head_k.astype(jnp.float32)
        value_f = head_v.astype(jnp.float32)

        def one_block(blk_args):
            query_blk, blk_index = blk_args
            query_pos = blk_index * blk_len + jnp.arange(blk_len, dtype=jnp.int32)
            scores = jnp.einsum('qmd,kmd->mqk', query_blk.astype(jnp.float32), key_f) * HEAD ** (-0.5)
            allowed = (positions // SPAN)[None, :] <= (query_pos // SPAN)[:, None]
            top_val = lax.optimization_barrier(jnp.max(jnp.where(allowed, scores, -jnp.inf), axis=-1, keepdims=True))
            expo_vals = jnp.where(allowed, jnp.exp(scores - top_val), 0.0)
            sums = lax.optimization_barrier(jnp.sum(expo_vals, axis=-1))
            rounded = lax.optimization_barrier(expo_vals.astype(jnp.bfloat16)).astype(jnp.float32)
            accum = jnp.einsum('mqk,ke->mqe', rounded, value_f)
            return accum[0] / sums[0][:, None] - head_lam * accum[1] / sums[1][:, None]
        blocks_out = lax.map(one_block, (head_q.reshape(blk_count, blk_len, 2, HEAD), jnp.arange(blk_count, dtype=jnp.int32)))
        return blocks_out.reshape(total_rows, value_dim)
    attn = lax.map(one_head, (queries, keys_all, values, head_lambda))
    mean_sq = lax.optimization_barrier(jnp.mean(attn * attn, axis=-1, keepdims=True))
    normed = (attn * lax.rsqrt(mean_sq + 1e-06) * sub_gain).astype(jnp.bfloat16)
    normed = normed.transpose(1, 0, 2).reshape(total_rows, head_count * value_dim)
    group_cols = head_count * value_dim // N_TP
    summed = jnp.zeros((total_rows, w_out.shape[1]), jnp.float32)
    for group in range(N_TP):
        partial_out = jnp.dot(normed[:, group * group_cols:(group + 1) * group_cols], w_out[group * group_cols:(group + 1) * group_cols], preferred_element_type=jnp.float32)
        summed = summed + lax.optimization_barrier(partial_out.astype(jnp.bfloat16)).astype(jnp.float32)
    return summed.astype(jnp.bfloat16)

def reference(tokens, w_query, w_key, w_value, w_out, head_lambda, sub_gain):
    outputs = []
    for seq_index in range(tokens.shape[1]):
        outputs.append(one_sequence(tokens[:, seq_index], w_query, w_key, w_value, w_out, head_lambda, sub_gain))
    return jnp.stack(outputs, axis=1)
```

```python
import functools

import jax
import jax.numpy as jnp
from jax import lax
from jax.experimental import pallas as pl
from jax.experimental.pallas import tpu as pltpu
from jax.sharding import PartitionSpec as P

SPAN = 64
NEG_FILL = -1e30
EPS_NORM = 1e-06
MESH = pl.DeviceIdType.MESH


def attend_kernel(
    n_sp,
    seqs,
    lam_ref,
    gain_ref,
    joined,
    out_ref,
    qbuf,
    kvbuf,
    ostage,
    lam_buf,
    qpad,
    top,
    acc,
    kv_sem,
    q_sem,
    o_sem,
    kv_send,
    q_send,
    o_send,
    fwd_core,
    fwd_chip,
    lam_sem,
):
    groups, _, rows, cols = joined.shape
    vdim = gain_ref.shape[1]
    head_dim = vdim // 2
    heads_here = cols // (3 * vdim)
    n_pairs = seqs * heads_here
    n_reg = n_sp // 2
    half = groups // 2
    chunk = half * rows
    tok_rows = groups * rows

    z = lax.axis_index("sp")
    tp = lax.axis_index("tp")
    core = lax.rem(tp, 2)
    chip_base = tp - core
    region = z // 2
    odd = lax.rem(z, 2)
    source_core = lax.rem(region, 2)
    pair = region // 2
    home_head, home_seq = pair // seqs, lax.rem(pair, seqs)
    rank = odd * 2 + core

    def dev(zz, cc):
        return {"sp": zz, "tp": chip_base + cc}

    def remote(src, dst, send, recv, zz, cc):
        return pltpu.make_async_remote_copy(
            src_ref=src, dst_ref=dst, send_sem=send, recv_sem=recv, device_id=dev(zz, cc), device_id_type=MESH
        )

    def entry_of(reg, zz):
        ahead = lax.rem(reg - zz // 2 + n_reg, n_reg)
        up = jnp.logical_or(ahead < n_reg // 2, jnp.logical_and(ahead == n_reg // 2, lax.rem(zz, 2) == 1))
        return jnp.where(ahead == 0, zz, jnp.where(up, 2 * reg, 2 * reg + 1))

    barrier = pltpu.get_barrier_semaphore()

    def greet(i, carry):
        zz, cc = i // 2, lax.rem(i, 2)

        @pl.when(jnp.logical_or(zz != z, cc != core))
        def _():
            pl.semaphore_signal(barrier, inc=1, device_id=dev(zz, cc), device_id_type=MESH)

        return carry

    lax.fori_loop(0, 2 * n_sp, greet, 0)
    pl.semaphore_wait(barrier, 2 * n_sp - 1)

    lam_copy = remote(lam_ref, lam_buf, lam_sem.at[0], lam_sem.at[1], z, 1 - core)
    lam_copy.start()

    def kv_src(k):
        head, seq = k // seqs, k % seqs
        return joined.at[:, seq, :, 2 * vdim * head : 2 * vdim * (head + 1)]

    for k in range(n_pairs):
        reg = 2 * k + core
        ent = entry_of(reg, z)
        here = ent == z

        @pl.when(here)
        def _():
            pltpu.make_async_copy(kv_src(k), kvbuf.at[z], kv_sem.at[z]).start()

        @pl.when(jnp.logical_not(here))
        def _():
            remote(kv_src(k), kvbuf.at[z], kv_send.at[k], kv_sem.at[z], ent, core).start()

    def q_src(k, b):
        head, seq = k // seqs, k % seqs
        first = (2 * heads_here + head) * vdim
        return joined.at[half * b : half * (b + 1), seq, :, first : first + vdim]

    def q_place(b):
        t = 2 * z + b
        u = lax.rem(t, 8)
        rk = jnp.where(u < 4, u, 7 - u)
        return rk // 2, lax.rem(rk, 2), (t // 8) * 2 + u // 4

    for b in range(2):
        rz, rc, slot = q_place(b)
        for k in range(n_pairs):
            zz = 2 * (2 * k + core) + rz
            here = jnp.logical_and(zz == z, rc == core)

            @pl.when(here)
            def _():
                pltpu.make_async_copy(q_src(k, b), qbuf.at[slot], q_sem.at[slot]).start()

            @pl.when(jnp.logical_not(here))
            def _():
                remote(q_src(k, b), qbuf.at[slot], q_send.at[2 * k + b], q_sem.at[slot], zz, rc).start()

    def arrive(n, carry):
        d = (n + 1) // 2
        zz = lax.rem(z + jnp.where(lax.rem(n, 2) == 1, d, n_sp - d), n_sp)
        pltpu.make_async_copy(kvbuf.at[zz], kvbuf.at[zz], kv_sem.at[zz]).wait()

        @pl.when(core == source_core)
        def _():
            @pl.when(entry_of(region, zz) == z)
            def _():
                remote(kvbuf.at[zz], kvbuf.at[zz], fwd_chip.at[zz], kv_sem.at[zz], z + 1 - 2 * odd, core).start()

            remote(kvbuf.at[zz], kvbuf.at[zz], fwd_core.at[zz], kv_sem.at[zz], z, 1 - core).start()

        return carry

    lax.fori_loop(0, n_sp, arrive, 0)
    lam_copy.wait()

    step_shards = 2
    step_keys = step_shards * tok_rows
    lam_rows = jnp.where(core == source_core, lam_ref[...], lam_buf[...])
    lam_row = lam_rows[0:1]
    for head in range(1, heads_here):
        lam_row = jnp.where(home_head == head, lam_rows[head : head + 1], lam_row)
    gain = gain_ref[...]
    lanes = lax.broadcasted_iota(jnp.int32, (chunk, vdim), 1)
    ones = jnp.ones((step_keys, vdim), jnp.bfloat16)

    def key_step(j, first_row):
        kv = kvbuf[pl.ds(j * step_shards, step_shards)].reshape(step_keys, 2 * vdim)
        keys = kv[:, :vdim]
        vals = jnp.concatenate([kv[:, vdim:], ones], axis=1)
        for m in range(2):
            here = slice(m * chunk, (m + 1) * chunk)
            scores = lax.dot_general(
                qpad[here], keys, (((1,), (1,)), ((), ())), preferred_element_type=jnp.float32
            )
            if first_row is not None:
                key_pos = j * step_keys + lax.broadcasted_iota(jnp.int32, (chunk, step_keys), 1)
                query_pos = first_row + lax.broadcasted_iota(jnp.int32, (chunk, step_keys), 0)
                scores = jnp.where(key_pos // SPAN <= query_pos // SPAN, scores, NEG_FILL)
            old = top[here]
            new = jnp.maximum(old, jnp.max(scores, axis=1, keepdims=True))
            expo = jnp.exp(scores - new[:, :1]).astype(jnp.bfloat16)
            factor = jnp.exp(old - new)
            acc[here] = acc[here] * jnp.concatenate([factor, factor], axis=1) + jnp.dot(
                expo, vals, preferred_element_type=jnp.float32
            )
            top[here] = new

    def o_dst(pr, b):
        head, seq = pr // seqs, lax.rem(pr, seqs)
        return out_ref.at[pl.ds(b * half, half), seq, :, pl.ds(pl.multiple_of(head * vdim, vdim), vdim)]

    def one_chunk(n, carry):
        t = (n // 2) * 8 + jnp.where(lax.rem(n, 2) == 1, 7 - rank, rank)
        pltpu.make_async_copy(qbuf.at[n], qbuf.at[n], q_sem.at[n]).wait()
        query = (qbuf[n].reshape(chunk, vdim).astype(jnp.float32) * head_dim ** (-0.5))
        qpad[:chunk] = jnp.where(lanes < head_dim, query, 0.0).astype(jnp.bfloat16)
        qpad[chunk:] = jnp.where(lanes < head_dim, 0.0, query).astype(jnp.bfloat16)
        top[...] = jnp.full(top.shape, NEG_FILL, jnp.float32)
        acc[...] = jnp.zeros(acc.shape, jnp.float32)
        full = (t * chunk) // step_keys

        def body(j, c):
            key_step(j, None)
            return c

        lax.fori_loop(0, full, body, 0)
        key_step(full, t * chunk)
        first, second = acc[:chunk], acc[chunk:]
        attn = first[:, :vdim] / first[:, vdim:] - lam_row * second[:, :vdim] / second[:, vdim:]
        mean_sq = jnp.mean(attn * attn, axis=1, keepdims=True)
        normed = attn * lax.rsqrt(mean_sq + EPS_NORM) * gain
        ostage[n] = normed.astype(jnp.bfloat16).reshape(half, rows, vdim)
        b, zz = lax.rem(t, 2), t // 2
        here = jnp.logical_and(zz == z, core == source_core)

        @pl.when(here)
        def _():
            pltpu.make_async_copy(ostage.at[n], o_dst(pair, b), o_sem.at[2 * pair + b]).start()

        @pl.when(jnp.logical_not(here))
        def _():
            remote(ostage.at[n], o_dst(pair, b), o_send.at[n], o_sem.at[2 * pair + b], zz, source_core).start()

        return carry

    lax.fori_loop(0, n_sp // 2, one_chunk, 0)

    for k in range(n_pairs):
        for b in range(2):
            pltpu.make_async_copy(o_dst(jnp.int32(k), b), o_dst(jnp.int32(k), b), o_sem.at[2 * k + b]).wait()

    for k in range(n_pairs):
        @pl.when(entry_of(2 * k + core, z) != z)
        def _():
            remote(kv_src(k), kvbuf.at[z], kv_send.at[k], kv_sem.at[z], z, core).wait_send()

        for b in range(2):
            rz, rc, slot = q_place(b)

            @pl.when(jnp.logical_or(2 * (2 * k + core) + rz != z, rc != core))
            def _():
                remote(q_src(k, b), qbuf.at[slot], q_send.at[2 * k + b], q_sem.at[slot], z, core).wait_send()

    def drain(n, carry):
        t = (n // 2) * 8 + jnp.where(lax.rem(n, 2) == 1, 7 - rank, rank)

        @pl.when(jnp.logical_or(t // 2 != z, core != source_core))
        def _():
            remote(ostage.at[n], ostage.at[n], o_send.at[n], q_sem.at[n], z, core).wait_send()

        return carry

    lax.fori_loop(0, n_sp // 2, drain, 0)

    @pl.when(core == source_core)
    def _():
        def sent(zz, carry):
            @pl.when(entry_of(region, zz) == z)
            def _():
                remote(kvbuf.at[zz], kvbuf.at[zz], fwd_chip.at[zz], kv_sem.at[zz], z, core).wait_send()

            remote(kvbuf.at[zz], kvbuf.at[zz], fwd_core.at[zz], kv_sem.at[zz], z, core).wait_send()
            return carry

        lax.fori_loop(0, n_sp, sent, 0)


def attend(joined, head_lambda, sub_gain, n_sp):
    groups, seqs, rows, cols = joined.shape
    heads_here = head_lambda.shape[0]
    vdim = sub_gain.shape[0]
    half = groups // 2
    chunk = half * rows
    n_pairs = seqs * heads_here
    n_chunks = n_sp // 2
    lam = jnp.broadcast_to(jnp.pad(head_lambda, (0, 8 - heads_here))[:, None], (8, vdim))
    dma = pltpu.SemaphoreType.DMA
    return pl.pallas_call(
        functools.partial(attend_kernel, n_sp, seqs),
        name="attend",
        out_shape=jax.ShapeDtypeStruct((groups, seqs, rows, heads_here * vdim), jnp.bfloat16),
        in_specs=[
            pl.BlockSpec(memory_space=pltpu.VMEM),
            pl.BlockSpec(memory_space=pltpu.VMEM),
            pl.BlockSpec(memory_space=pltpu.HBM),
        ],
        out_specs=pl.BlockSpec(memory_space=pltpu.HBM),
        scratch_shapes=[
            pltpu.VMEM((n_chunks, half, rows, vdim), jnp.bfloat16),
            pltpu.VMEM((n_sp, groups, rows, 2 * vdim), jnp.bfloat16),
            pltpu.VMEM((n_chunks, half, rows, vdim), jnp.bfloat16),
            pltpu.VMEM((8, vdim), jnp.float32),
            pltpu.VMEM((2 * chunk, vdim), jnp.bfloat16),
            pltpu.VMEM((2 * chunk, vdim), jnp.float32),
            pltpu.VMEM((2 * chunk, 2 * vdim), jnp.float32),
            dma((n_sp,)),
            dma((n_chunks,)),
            dma((2 * n_pairs,)),
            dma((n_pairs,)),
            dma((2 * n_pairs,)),
            dma((n_chunks,)),
            dma((n_sp,)),
            dma((n_sp,)),
            dma((2,)),
        ],
        compiler_params=pltpu.CompilerParams(
            collective_id=0, has_side_effects=True, vmem_limit_bytes=48 * 1024 * 1024
        ),
    )(lam, sub_gain[None, :], joined)


def on_device(n_sp, tokens, w_query, w_key, w_value, w_out, head_lambda, sub_gain):
    heads_here = head_lambda.shape[0]
    vdim = sub_gain.shape[0]
    parts = []
    for head in range(heads_here):
        cut = slice(head * vdim, (head + 1) * vdim)
        parts += [w_key[:, cut], w_value[:, cut]]
    w_joined = jnp.concatenate(parts + [w_query], axis=1)
    turned = jnp.transpose(tokens, (1, 0, 2))
    gathered = lax.all_gather(turned, "tp", axis=0, tiled=False)
    joined = jnp.dot(gathered, w_joined, preferred_element_type=jnp.float32).astype(jnp.bfloat16)
    normed = attend(joined, head_lambda, sub_gain, n_sp)
    partial = jnp.dot(normed, w_out, preferred_element_type=jnp.float32).astype(jnp.bfloat16)
    arrived = lax.all_to_all(partial, "tp", split_axis=0, concat_axis=0, tiled=True)
    summed = arrived.astype(jnp.float32).sum(axis=0).astype(jnp.bfloat16)
    return jnp.transpose(summed, (1, 0, 2))


def solution(mesh):
    return jax.shard_map(
        functools.partial(on_device, mesh.shape["sp"]),
        mesh=mesh,
        in_specs=(
            P(("grp", "sp", "tp"), None, None),
            P(None, "tp"),
            P(None, "tp"),
            P(None, "tp"),
            P("tp", None),
            P("tp"),
            P(),
        ),
        out_specs=P(("grp", "sp", "tp"), None, None),
        check_vma=False,
    )
```

```python
import functools

import jax
import jax.numpy as jnp
from jax import lax
from jax.experimental import pallas as pl
from jax.experimental.pallas import tpu as pltpu
from jax.sharding import PartitionSpec as P

SPAN = 64
NEG_FILL = -1e30
EPS_NORM = 1e-06
LEAD = 2
QUOTA = 5
MESH = pl.DeviceIdType.MESH


def layer_kernel(
    n_sp,
    turned,
    wq_ref,
    wk_ref,
    wv_ref,
    wo_ref,
    lam_ref,
    gain_ref,
    out_ref,
    tok,
    jbuf,
    qbuf,
    kvbuf,
    ostage,
    nbuf,
    lam_buf,
    qpad,
    top,
    acc,
    mine,
    sib_out,
    sib_in,
    xs,
    xr,
    ag_recv,
    ag_half,
    ag_send,
    kv_sem,
    q_sem,
    o_sem,
    kv_send,
    q_send,
    o_send,
    fwd_core,
    fwd_chip,
    lam_sem,
    sib_send,
    sib_recv,
    x_send,
    x_recv,
):
    seqs, groups, rows, _ = jbuf.shape
    width = tok.shape[3]
    vdim = gain_ref.shape[1]
    head_dim = vdim // 2
    heads_here = wq_ref.shape[1] // vdim
    n_pairs = seqs * heads_here
    n_reg = n_sp // 2
    n_x = groups // 2
    half = groups // 2
    chunk = half * rows
    tok_rows = groups * rows
    n_chunks = n_sp // 2

    z = lax.axis_index("sp")
    tp = lax.axis_index("tp")
    core = lax.rem(tp, 2)
    x = tp // 2
    region = z // 2
    odd = lax.rem(z, 2)
    source_core = lax.rem(region, 2)
    is_primary = core == source_core
    pair = region // 2
    home_head, home_seq = pair // seqs, lax.rem(pair, seqs)
    rank = odd * 2 + core

    def tp_of(ahead, cc):
        return 2 * lax.rem(x + ahead + n_x, n_x) + cc

    def to(src, dst, send, recv, zz, tt):
        return pltpu.make_async_remote_copy(
            src_ref=src,
            dst_ref=dst,
            send_sem=send,
            recv_sem=recv,
            device_id={"sp": zz, "tp": tt},
            device_id_type=MESH,
        )

    def remote(src, dst, send, recv, zz, cc):
        return to(src, dst, send, recv, zz, 2 * x + cc)

    def got(ref, sem):
        pltpu.make_async_copy(ref, ref, sem).wait()

    def entry_of(reg, zz):
        ahead = lax.rem(reg - zz // 2 + n_reg, n_reg)
        up = jnp.logical_or(ahead < n_reg // 2, jnp.logical_and(ahead == n_reg // 2, lax.rem(zz, 2) == 1))
        return jnp.where(ahead == 0, zz, jnp.where(up, 2 * reg, 2 * reg + 1))

    barrier = pltpu.get_barrier_semaphore()

    def greet(i, carry):
        zz, cc = i // 2, lax.rem(i, 2)

        @pl.when(jnp.logical_or(zz != z, cc != core))
        def _():
            pl.semaphore_signal(barrier, inc=1, device_id={"sp": zz, "tp": 2 * x + cc}, device_id_type=MESH)

        return carry

    for ahead in (1, -1):
        pl.semaphore_signal(barrier, inc=1, device_id={"sp": z, "tp": tp_of(ahead, core)}, device_id_type=MESH)
    lax.fori_loop(0, 2 * n_sp, greet, 0)
    pl.semaphore_wait(barrier, 2 * n_sp + 1)

    low, high = slice(0, rows // 2), slice(rows // 2, rows)

    def gather_copies(s):
        own, back, fore, far = tp, tp_of(-1, core), tp_of(1, core), tp_of(2, core)

        def send(i, src, dst, sem, tt):
            return to(src, dst, ag_send.at[8 * s + i], sem, z, tt)

        sib = 2 * x + 1 - core

        def full(i, t, tt):
            return send(i, tok.at[s, t], tok.at[s, t], ag_recv.at[groups * s + t], tt)

        return (
            lambda: send(0, turned.at[s], tok.at[s, own], ag_recv.at[groups * s + own], fore),
            lambda: send(1, turned.at[s], tok.at[s, own], ag_recv.at[groups * s + own], back),
            lambda: send(2, turned.at[s], tok.at[s, own], ag_recv.at[groups * s + own], sib),
            lambda: send(3, tok.at[s, back, low], tok.at[s, back, low], ag_half.at[2 * s], fore),
            lambda: send(4, tok.at[s, fore, high], tok.at[s, fore, high], ag_half.at[2 * s + 1], back),
            lambda: full(5, back, sib),
            lambda: full(6, fore, sib),
            lambda: full(7, far, sib),
        )

    def gather_start(s):
        pltpu.make_async_copy(turned.at[s], tok.at[s, tp], ag_recv.at[groups * s + tp]).start()
        for copy in gather_copies(s)[:3]:
            copy().start()

    def gather_near(s):
        copies = gather_copies(s)
        for i, ahead in enumerate((-1, 1)):
            t = tp_of(ahead, core)
            got(tok.at[s, t], ag_recv.at[groups * s + t])
            copies[3 + i]().start()
            copies[5 + i]().start()

    def gather_far(s):
        t = tp_of(2, core)
        got(tok.at[s, t, low], ag_half.at[2 * s])
        got(tok.at[s, t, high], ag_half.at[2 * s + 1])
        gather_copies(s)[7]().start()
        got(tok.at[s, tp], ag_recv.at[groups * s + tp])
        for ahead in (0, 1, -1, 2):
            t = tp_of(ahead, 1 - core)
            got(tok.at[s, t], ag_recv.at[groups * s + t])

    def project(s):
        def tile(i, carry):
            at = pl.ds(i * half, half)
            block = tok[s, at].reshape(chunk, width)
            for ref, first, step in ((wk_ref, 0, 2 * vdim), (wv_ref, vdim, 2 * vdim), (wq_ref, n_pairs * vdim, vdim)):
                done = jnp.dot(block, ref[...], preferred_element_type=jnp.float32).astype(jnp.bfloat16)
                for head in range(heads_here):
                    jbuf[s, at, :, first + head * step : first + head * step + vdim] = done[
                        :, head * vdim : (head + 1) * vdim
                    ].reshape(half, rows, vdim)
            return carry

        lax.fori_loop(0, 2, tile, 0)

    def kv_src(k):
        head, seq = k // seqs, k % seqs
        return jbuf.at[seq, :, :, 2 * vdim * head : 2 * vdim * (head + 1)]

    def q_src(k, b):
        head, seq = k // seqs, k % seqs
        first = (2 * heads_here + head) * vdim
        return jbuf.at[seq, half * b : half * (b + 1), :, first : first + vdim]

    def q_place(b):
        t = 2 * z + b
        u = lax.rem(t, 8)
        rk = jnp.where(u < 4, u, 7 - u)
        return rk // 2, lax.rem(rk, 2), (t // 8) * 2 + u // 4

    def q_copy(k, b):
        rz, rc, slot = q_place(b)
        zz = 2 * (2 * k + core) + rz
        here = jnp.logical_and(zz == z, rc == core)
        return here, slot, lambda: remote(q_src(k, b), qbuf.at[slot], q_send.at[2 * k + b], q_sem.at[slot], zz, rc)

    def kv_copy(k):
        ent = entry_of(2 * k + core, z)
        return ent == z, lambda: remote(kv_src(k), kvbuf.at[z], kv_send.at[k], kv_sem.at[z], ent, core)

    def send_queries(s):
        for k in range(s, n_pairs, seqs):
            for b in range(2):
                here, slot, copy = q_copy(k, b)

                @pl.when(here)
                def _():
                    qbuf[slot] = q_src(k, b)[...]

                @pl.when(jnp.logical_not(here))
                def _():
                    copy().start()

    def send_keys():
        for k in range(n_pairs):
            here, _ = kv_copy(k)

            @pl.when(here)
            def _():
                remote(kv_src(k), kvbuf.at[z], fwd_chip.at[z], kv_sem.at[z], z + 1 - 2 * odd, core).start()
                remote(kv_src(k), kvbuf.at[z], fwd_core.at[z], kv_sem.at[z], z, 1 - core).start()
                kvbuf[z] = kv_src(k)[...]

        for near in (True, False):
            for k in range(n_pairs):
                here, copy = kv_copy(k)
                ahead = lax.rem(2 * k + core - region + n_reg, n_reg)
                close = jnp.minimum(ahead, n_reg - ahead) <= n_reg // 4

                @pl.when(jnp.logical_and(jnp.logical_not(here), close if near else jnp.logical_not(close)))
                def _():
                    copy().start()

    lam_copy = remote(lam_ref, lam_buf, lam_sem.at[0], lam_sem.at[1], z, 1 - core)
    lam_copy.start()
    gather_start(0)
    gather_near(0)
    gather_start(1)
    gather_far(0)
    project(0)
    send_queries(0)
    gather_near(1)
    gather_far(1)
    project(1)
    send_queries(1)
    send_keys()
    lam_copy.wait()

    lanes = lax.broadcasted_iota(jnp.int32, (chunk, vdim), 1)
    step_keys = 2 * tok_rows
    ones = jnp.ones((step_keys, vdim), jnp.bfloat16)

    def chunk_of(n):
        return (n // 2) * 8 + jnp.where(lax.rem(n, 2) == 1, 7 - rank, rank)

    def local_chunk(n):
        t = chunk_of(n)
        return jnp.logical_and(t // 2 == z, is_primary)

    def ready(n, carry):
        @pl.when(jnp.logical_not(local_chunk(n)))
        def _():
            got(qbuf.at[n], q_sem.at[n])

        query = qbuf[n].reshape(chunk, vdim).astype(jnp.float32) * head_dim ** (-0.5)
        qpad[n, :chunk] = jnp.where(lanes < head_dim, query, 0.0).astype(jnp.bfloat16)
        qpad[n, chunk:] = jnp.where(lanes < head_dim, 0.0, query).astype(jnp.bfloat16)
        top[n] = jnp.full(top.shape[1:], NEG_FILL, jnp.float32)
        acc[n] = jnp.zeros(acc.shape[1:], jnp.float32)
        return carry

    def block(n, reg, first_row):
        kv = kvbuf[pl.ds(2 * reg, 2)].reshape(step_keys, 2 * vdim)
        keys = kv[:, :vdim]
        vals = jnp.concatenate([kv[:, vdim:], ones], axis=1)
        for m in range(2):
            here = slice(m * chunk, (m + 1) * chunk)
            scores = lax.dot_general(
                qpad[n, here], keys, (((1,), (1,)), ((), ())), preferred_element_type=jnp.float32
            )
            if first_row is not None:
                row = first_row + lax.broadcasted_iota(jnp.int32, (chunk, 1), 0)
                limit = (row // SPAN + 1) * SPAN
                key = lax.broadcasted_iota(jnp.int32, (chunk, step_keys), 1)
                scores = jnp.where(key < limit, scores, NEG_FILL)
            old = top[n, here]
            new = jnp.maximum(old, jnp.max(scores, axis=1, keepdims=True))
            expo = jnp.exp(scores - new[:, :1]).astype(jnp.bfloat16)
            factor = jnp.exp(old - new)
            acc[n, here] = acc[n, here] * jnp.concatenate([factor, factor], axis=1) + jnp.dot(
                expo, vals, preferred_element_type=jnp.float32
            )
            top[n, here] = new

    def own_shard(zz):
        return jnp.logical_and(zz == z, is_primary)

    def side(direct, lap):
        above = (odd == 1) if direct else (odd == 0)
        return lax.rem(region + jnp.where(above, lap, n_reg - lap), n_reg), above

    def shard_at(direct, k):
        lap, second = (k + 1) // 2, lax.rem(k + 1, 2)
        reg, above = side(direct, lap)
        far = jnp.where(k == n_reg - 1, 0, second)
        own = 2 * region + (odd if direct else 1 - odd)
        return jnp.where(k == 0, own, 2 * reg + jnp.where(above, far, 1 - far))

    def region_at(i):
        lap = (i + 1) // 2
        return jnp.where(lax.rem(i, 2) == 1, side(True, lap)[0], side(False, lap)[0])

    def use(p, c):
        reg, n = region_at(p // n_chunks), lax.rem(p, n_chunks)

        @pl.when(n > reg)
        def _():
            block(n, reg, None)

        @pl.when(n == reg)
        def _():
            block(n, reg, lax.rem(chunk_of(n), 4) * chunk)

        return c

    def take(zz, direct):
        @pl.when(jnp.logical_not(own_shard(zz)))
        def _():
            got(kvbuf.at[zz], kv_sem.at[zz])

            @pl.when(is_primary)
            def _():
                if direct:
                    remote(
                        kvbuf.at[zz], kvbuf.at[zz], fwd_chip.at[zz], kv_sem.at[zz], z + 1 - 2 * odd, core
                    ).start()
                remote(kvbuf.at[zz], kvbuf.at[zz], fwd_core.at[zz], kv_sem.at[zz], z, 1 - core).start()

    def arrive(i, used):
        @pl.when(i < n_reg)
        def _():
            take(shard_at(True, i), True)

        @pl.when(i == LEAD)
        def _():
            lax.fori_loop(0, n_chunks, ready, 0)

        def spend(used, done):
            whole = jnp.where(done < 1, 0, jnp.where(done == n_reg, n_reg, 2 * ((done - 1) // 2) + 2))
            whole = jnp.where(done == n_reg - 1, n_reg - 1, whole)
            upto = jnp.maximum(jnp.minimum(whole * n_chunks, used + QUOTA), used)
            lax.fori_loop(used, upto, use, 0)
            return upto

        used = spend(used, i - LEAD)

        @pl.when(i >= LEAD)
        def _():
            take(shard_at(False, i - LEAD), False)

        return spend(used, i - LEAD + 1)

    used = lax.fori_loop(0, n_reg + LEAD, arrive, jnp.int32(0))
    lax.fori_loop(used, n_reg * n_chunks, use, 0)

    lam_rows = jnp.where(is_primary, lam_ref[...], lam_buf[...])
    lam_row = lam_rows[0:1]
    for head in range(1, heads_here):
        lam_row = jnp.where(home_head == head, lam_rows[head : head + 1], lam_row)
    gain = gain_ref[...]

    def o_dst(pr, b):
        head, seq = pr // seqs, lax.rem(pr, seqs)
        return nbuf.at[pl.ds(b * n_x // 2, n_x // 2), :, seq, :, pl.ds(pl.multiple_of(head * vdim, vdim), vdim)]

    def finish(n, carry):
        t = chunk_of(n)
        first, second = acc[n, :chunk], acc[n, chunk:]
        attn = first[:, :vdim] / first[:, vdim:] - lam_row * second[:, :vdim] / second[:, vdim:]
        mean_sq = jnp.mean(attn * attn, axis=1, keepdims=True)
        normed = (attn * lax.rsqrt(mean_sq + EPS_NORM) * gain).astype(jnp.bfloat16).reshape(n_x // 2, 2, rows, vdim)
        b, zz = lax.rem(t, 2), t // 2
        here = local_chunk(n)
        ostage[n] = normed

        @pl.when(here)
        def _():
            o_dst(pair, b)[...] = normed

        @pl.when(jnp.logical_not(here))
        def _():
            remote(ostage.at[n], o_dst(pair, b), o_send.at[n], o_sem.at[2 * pair + b], zz, source_core).start()

        return carry

    lax.fori_loop(0, n_chunks, finish, 0)

    def partial(cc, s):
        block = nbuf[:, cc, s].reshape(n_x * rows, heads_here * vdim)
        done = jnp.dot(block, wo_ref[...], preferred_element_type=jnp.float32)
        return done.astype(jnp.bfloat16).reshape(n_x, rows, width)

    def sib_copy(s):
        return remote(sib_out.at[s], sib_in.at[s], sib_send.at[s], sib_recv.at[s], z, 1 - core)

    def both(s, ahead, part):
        to_x = lax.rem(x + ahead + n_x, n_x)
        return mine[s, to_x, part].astype(jnp.float32) + sib_in[s, to_x, part].astype(jnp.float32)

    ways = (1, -1, 1, -1, 1, -1)

    def x_copy(s, i):
        at = len(ways) * s + i
        return to(xs.at[at], xr.at[at], x_send.at[at], x_recv.at[at], z, tp_of(ways[i], core))

    def ship(s, i, value):
        xs[len(ways) * s + i] = value.astype(jnp.bfloat16)
        x_copy(s, i).start()

    def came(s, i):
        at = len(ways) * s + i
        got(xr.at[at], x_recv.at[at])
        return xr[at].astype(jnp.float32)

    def sum_start(s):
        for k in range(s, n_pairs, seqs):
            for b in range(2):
                here, _, _ = q_copy(k, b)

                @pl.when(jnp.logical_not(here))
                def _():
                    got(o_dst(jnp.int32(k), b), o_sem.at[2 * k + b])

        sib_out[s] = partial(1 - core, s)
        sib_copy(s).start()
        mine[s] = partial(core, s)
        got(sib_in.at[s], sib_recv.at[s])
        ship(s, 0, both(s, 2, low))
        ship(s, 1, both(s, 2, high))
        ship(s, 2, both(s, 1, high))
        ship(s, 3, both(s, -1, low))

    def sum_pass(s):
        ship(s, 4, both(s, 1, low) + came(s, 0))
        ship(s, 5, both(s, -1, high) + came(s, 1))

    def sum_end(s):
        out_ref[s, low] = (both(s, 0, low) + came(s, 3) + came(s, 4)).astype(jnp.bfloat16)
        out_ref[s, high] = (both(s, 0, high) + came(s, 2) + came(s, 5)).astype(jnp.bfloat16)

    sum_start(0)
    sum_pass(0)
    sum_start(1)
    sum_end(0)
    sum_pass(1)
    sum_end(1)

    for s in range(seqs):
        sib_copy(s).wait_send()
        for i in range(len(ways)):
            x_copy(s, i).wait_send()
    for s in range(seqs):
        for copy in gather_copies(s):
            copy().wait_send()
    for k in range(n_pairs):
        here, copy = kv_copy(k)

        @pl.when(jnp.logical_not(here))
        def _():
            copy().wait_send()

        for b in range(2):
            q_here, _, q_sent = q_copy(k, b)

            @pl.when(jnp.logical_not(q_here))
            def _():
                q_sent().wait_send()

    def drain(n, carry):
        @pl.when(jnp.logical_not(local_chunk(n)))
        def _():
            remote(ostage.at[n], ostage.at[n], o_send.at[n], q_sem.at[n], z, 1 - core).wait_send()

        return carry

    lax.fori_loop(0, n_chunks, drain, 0)

    @pl.when(is_primary)
    def _():
        def sent(zz, carry):
            @pl.when(entry_of(region, zz) == z)
            def _():
                remote(kvbuf.at[zz], kvbuf.at[zz], fwd_chip.at[zz], kv_sem.at[zz], z, 1 - core).wait_send()

            remote(kvbuf.at[zz], kvbuf.at[zz], fwd_core.at[zz], kv_sem.at[zz], z, 1 - core).wait_send()
            return carry

        lax.fori_loop(0, n_sp, sent, 0)


def on_device(n_sp, n_tp, tokens, w_query, w_key, w_value, w_out, head_lambda, sub_gain):
    rows, seqs, width = tokens.shape
    heads_here = head_lambda.shape[0]
    vdim = sub_gain.shape[0]
    half = n_tp // 2
    chunk = half * rows
    n_pairs = seqs * heads_here
    n_chunks = n_sp // 2
    lam = jnp.broadcast_to(jnp.pad(head_lambda, (0, 8 - heads_here))[:, None], (8, vdim))
    turned = jnp.transpose(tokens, (1, 0, 2))
    dma = pltpu.SemaphoreType.DMA
    bf16, f32 = jnp.bfloat16, jnp.float32
    in_vmem = pl.BlockSpec(memory_space=pltpu.VMEM)
    out = pl.pallas_call(
        functools.partial(layer_kernel, n_sp),
        name="layer",
        out_shape=jax.ShapeDtypeStruct((seqs, rows, width), bf16),
        in_specs=[pl.BlockSpec(memory_space=pltpu.HBM)] + [in_vmem] * 6,
        out_specs=in_vmem,
        scratch_shapes=[
            pltpu.VMEM((seqs, n_tp, rows, width), bf16),
            pltpu.VMEM((seqs, n_tp, rows, 3 * heads_here * vdim), bf16),
            pltpu.VMEM((n_chunks, half, rows, vdim), bf16),
            pltpu.VMEM((n_sp, n_tp, rows, 2 * vdim), bf16),
            pltpu.VMEM((n_chunks, n_tp // 4, 2, rows, vdim), bf16),
            pltpu.VMEM((n_tp // 2, 2, seqs, rows, heads_here * vdim), bf16),
            pltpu.VMEM((8, vdim), f32),
            pltpu.VMEM((n_chunks, 2 * chunk, vdim), bf16),
            pltpu.VMEM((n_chunks, 2 * chunk, vdim), f32),
            pltpu.VMEM((n_chunks, 2 * chunk, 2 * vdim), f32),
            pltpu.VMEM((seqs, n_tp // 2, rows, width), bf16),
            pltpu.VMEM((seqs, n_tp // 2, rows, width), bf16),
            pltpu.VMEM((seqs, n_tp // 2, rows, width), bf16),
            pltpu.VMEM((6 * seqs, rows // 2, width), bf16),
            pltpu.VMEM((6 * seqs, rows // 2, width), bf16),
            dma((seqs * n_tp,)),
            dma((2 * seqs,)),
            dma((8 * seqs,)),
            dma((n_sp,)),
            dma((n_chunks,)),
            dma((2 * n_pairs,)),
            dma((n_pairs,)),
            dma((2 * n_pairs,)),
            dma((n_chunks,)),
            dma((n_sp,)),
            dma((n_sp,)),
            dma((2,)),
            dma((seqs,)),
            dma((seqs,)),
            dma((6 * seqs,)),
            dma((6 * seqs,)),
        ],
        compiler_params=pltpu.CompilerParams(
            collective_id=0, has_side_effects=True, vmem_limit_bytes=60 * 1024 * 1024
        ),
    )(turned, w_query, w_key, w_value, w_out, lam, sub_gain[None, :])
    return jnp.transpose(out, (1, 0, 2))


def solution(mesh):
    return jax.shard_map(
        functools.partial(on_device, mesh.shape["sp"], mesh.shape["tp"]),
        mesh=mesh,
        in_specs=(
            P(("grp", "sp", "tp"), None, None),
            P(None, "tp"),
            P(None, "tp"),
            P(None, "tp"),
            P("tp", None),
            P("tp"),
            P(),
        ),
        out_specs=P(("grp", "sp", "tp"), None, None),
        check_vma=False,
    )
```

```python
import functools

import jax
import jax.numpy as jnp
from jax import lax
from jax.experimental import pallas as pl
from jax.experimental.pallas import tpu as pltpu
from jax.sharding import PartitionSpec as P

SPAN = 64
NEG_FILL = -1e30
EPS_NORM = 1e-06
LEAD = 2
QUOTA = 2
MESH = pl.DeviceIdType.MESH


def layer_kernel(
    n_sp,
    turned,
    wq_ref,
    wk_ref,
    wv_ref,
    wo_ref,
    lam_ref,
    gain_ref,
    out_ref,
    tok,
    qj,
    kvj,
    qbuf,
    kvbuf,
    ostage,
    nbuf,
    lam_buf,
    qpad,
    top,
    acc,
    mine,
    sib_out,
    sib_in,
    xs,
    xr,
    ag_recv,
    ag_half,
    ag_send,
    kv_sem,
    q_sem,
    o_sem,
    kv_send,
    q_send,
    o_send,
    fwd_core,
    fwd_chip,
    lam_sem,
    sib_send,
    sib_recv,
    x_send,
    x_recv,
):
    seqs, groups, rows, width = tok.shape
    vdim = gain_ref.shape[1]
    head_dim = vdim // 2
    heads_here = wq_ref.shape[1] // vdim
    n_pairs = seqs * heads_here
    n_reg = n_sp // 2
    n_x = groups // 2
    half = groups // 2
    chunk = half * rows
    tok_rows = groups * rows
    n_chunks = n_sp // 2

    z = lax.axis_index("sp")
    tp = lax.axis_index("tp")
    core = lax.rem(tp, 2)
    x = tp // 2
    region = z // 2
    odd = lax.rem(z, 2)
    source_core = lax.rem(region, 2)
    is_primary = core == source_core
    pair = region // 2
    home_head, home_seq = pair // seqs, lax.rem(pair, seqs)
    rank = odd * 2 + core

    def tp_of(ahead, cc):
        return 2 * lax.rem(x + ahead + n_x, n_x) + cc

    def to(src, dst, send, recv, zz, tt):
        return pltpu.make_async_remote_copy(
            src_ref=src,
            dst_ref=dst,
            send_sem=send,
            recv_sem=recv,
            device_id={"sp": zz, "tp": tt},
            device_id_type=MESH,
        )

    def remote(src, dst, send, recv, zz, cc):
        return to(src, dst, send, recv, zz, 2 * x + cc)

    def got(ref, sem):
        pltpu.make_async_copy(ref, ref, sem).wait()

    def entry_of(reg, zz):
        ahead = lax.rem(reg - zz // 2 + n_reg, n_reg)
        up = jnp.logical_or(ahead < n_reg // 2, jnp.logical_and(ahead == n_reg // 2, lax.rem(zz, 2) == 1))
        return jnp.where(ahead == 0, zz, jnp.where(up, 2 * reg, 2 * reg + 1))

    barrier = pltpu.get_barrier_semaphore()

    def greet(i, carry):
        zz, cc = i // 2, lax.rem(i, 2)

        @pl.when(jnp.logical_or(zz != z, cc != core))
        def _():
            pl.semaphore_signal(barrier, inc=1, device_id={"sp": zz, "tp": 2 * x + cc}, device_id_type=MESH)

        return carry

    for ahead in (1, -1):
        pl.semaphore_signal(barrier, inc=1, device_id={"sp": z, "tp": tp_of(ahead, core)}, device_id_type=MESH)
    lax.fori_loop(0, 2 * n_sp, greet, 0)
    pl.semaphore_wait(barrier, 2 * n_sp + 1)

    low, high = slice(0, rows // 2), slice(rows // 2, rows)

    def gather_copies(s):
        own, back, fore, far = tp, tp_of(-1, core), tp_of(1, core), tp_of(2, core)

        def send(i, src, dst, sem, tt):
            return to(src, dst, ag_send.at[8 * s + i], sem, z, tt)

        sib = 2 * x + 1 - core

        def full(i, t, tt):
            return send(i, tok.at[s, t], tok.at[s, t], ag_recv.at[groups * s + t], tt)

        return (
            lambda: send(0, turned.at[s], tok.at[s, own], ag_recv.at[groups * s + own], fore),
            lambda: send(1, turned.at[s], tok.at[s, own], ag_recv.at[groups * s + own], back),
            lambda: send(2, turned.at[s], tok.at[s, own], ag_recv.at[groups * s + own], sib),
            lambda: send(3, tok.at[s, back, low], tok.at[s, back, low], ag_half.at[2 * s], fore),
            lambda: send(4, tok.at[s, fore, high], tok.at[s, fore, high], ag_half.at[2 * s + 1], back),
            lambda: full(5, back, sib),
            lambda: full(6, fore, sib),
            lambda: full(7, far, sib),
        )

    def gather_start(s):
        pltpu.make_async_copy(turned.at[s], tok.at[s, tp], ag_recv.at[groups * s + tp]).start()
        for copy in gather_copies(s)[:3]:
            copy().start()

    def gather_near(s):
        copies = gather_copies(s)
        for i, ahead in enumerate((-1, 1)):
            t = tp_of(ahead, core)
            got(tok.at[s, t], ag_recv.at[groups * s + t])
            copies[3 + i]().start()
            copies[5 + i]().start()

    def gather_far(s):
        t = tp_of(2, core)
        got(tok.at[s, t, low], ag_half.at[2 * s])
        got(tok.at[s, t, high], ag_half.at[2 * s + 1])
        gather_copies(s)[7]().start()
        got(tok.at[s, tp], ag_recv.at[groups * s + tp])
        for ahead in (0, 1, -1, 2):
            t = tp_of(ahead, 1 - core)
            got(tok.at[s, t], ag_recv.at[groups * s + t])

    def project(s):
        def tile(i, carry):
            block = tok[s, pl.ds(i * half, half)].reshape(chunk, width)
            at = pl.ds(pl.multiple_of(i * chunk, chunk), chunk)
            keys = jnp.dot(block, wk_ref[...], preferred_element_type=jnp.float32).astype(jnp.bfloat16)
            vals = jnp.dot(block, wv_ref[...], preferred_element_type=jnp.float32).T.astype(jnp.bfloat16)
            queries = jnp.dot(block, wq_ref[...], preferred_element_type=jnp.float32).astype(jnp.bfloat16)
            for head in range(heads_here):
                k, cut = head * seqs + s, slice(head * vdim, (head + 1) * vdim)
                qj[k, at] = queries[:, cut]
                kvj[k, 0, at] = keys[:, cut]
                for part in range(chunk // vdim):
                    first = pl.multiple_of(i * chunk + part * vdim, vdim)
                    kvj[k, 1, pl.ds(first, vdim)] = vals[cut, part * vdim : (part + 1) * vdim]
            return carry

        lax.fori_loop(0, 2, tile, 0)

    def kv_src(k):
        return kvj.at[k]

    def q_src(k, b):
        return qj.at[k, b * chunk : (b + 1) * chunk]

    def q_place(b):
        t = 2 * z + b
        u = lax.rem(t, 8)
        rk = jnp.where(u < 4, u, 7 - u)
        return rk // 2, lax.rem(rk, 2), (t // 8) * 2 + u // 4

    def q_copy(k, b):
        rz, rc, slot = q_place(b)
        zz = 2 * (2 * k + core) + rz
        here = jnp.logical_and(zz == z, rc == core)
        return here, slot, lambda: remote(q_src(k, b), qbuf.at[slot], q_send.at[2 * k + b], q_sem.at[slot], zz, rc)

    def kv_copy(k):
        ent = entry_of(2 * k + core, z)
        return ent == z, lambda: remote(kv_src(k), kvbuf.at[z], kv_send.at[k], kv_sem.at[z], ent, core)

    def send_queries(s):
        for k in range(s, n_pairs, seqs):
            for b in range(2):
                here, slot, copy = q_copy(k, b)

                @pl.when(here)
                def _():
                    qbuf[slot] = q_src(k, b)[...]

                @pl.when(jnp.logical_not(here))
                def _():
                    copy().start()

    def send_keys():
        for k in range(n_pairs):
            here, _ = kv_copy(k)

            @pl.when(here)
            def _():
                remote(kv_src(k), kvbuf.at[z], fwd_chip.at[z], kv_sem.at[z], z + 1 - 2 * odd, core).start()
                remote(kv_src(k), kvbuf.at[z], fwd_core.at[z], kv_sem.at[z], z, 1 - core).start()
                kvbuf[z] = kv_src(k)[...]

        for near in (True, False):
            for k in range(n_pairs):
                here, copy = kv_copy(k)
                ahead = lax.rem(2 * k + core - region + n_reg, n_reg)
                close = jnp.minimum(ahead, n_reg - ahead) <= n_reg // 4

                @pl.when(jnp.logical_and(jnp.logical_not(here), close if near else jnp.logical_not(close)))
                def _():
                    copy().start()

    lam_copy = remote(lam_ref, lam_buf, lam_sem.at[0], lam_sem.at[1], z, 1 - core)
    lam_copy.start()
    gather_start(0)
    gather_near(0)
    gather_start(1)
    gather_far(0)
    project(0)
    send_queries(0)
    gather_near(1)
    gather_far(1)
    project(1)
    send_queries(1)
    send_keys()
    lam_copy.wait()

    channel = lax.broadcasted_iota(jnp.int32, (vdim, chunk), 0)
    ones = jnp.ones((acc.shape[1] - vdim, tok_rows), jnp.bfloat16)

    def chunk_of(n):
        return (n // 2) * 8 + jnp.where(lax.rem(n, 2) == 1, 7 - rank, rank)

    def local_chunk(n):
        t = chunk_of(n)
        return jnp.logical_and(t // 2 == z, is_primary)

    def ready(n, carry):
        @pl.when(jnp.logical_not(local_chunk(n)))
        def _():
            got(qbuf.at[n], q_sem.at[n])

        query = qbuf[n].astype(jnp.float32).T * head_dim ** (-0.5)
        qpad[n, :, :chunk] = jnp.where(channel < head_dim, query, 0.0).astype(jnp.bfloat16)
        qpad[n, :, chunk:] = jnp.where(channel < head_dim, 0.0, query).astype(jnp.bfloat16)
        top[n] = jnp.full(top.shape[1:], NEG_FILL, jnp.float32)
        acc[n] = jnp.zeros(acc.shape[1:], jnp.float32)
        return carry

    def block(n, zz, first_row):
        turned_vals = kvbuf[zz, 1].reshape(tok_rows // vdim, vdim, vdim)
        vals = jnp.concatenate([turned_vals[i] for i in range(tok_rows // vdim)], axis=1)
        vals = jnp.concatenate([vals, ones], axis=0)
        scores = jnp.dot(kvbuf[zz, 0], qpad[n], preferred_element_type=jnp.float32)
        if first_row is not None:
            column = lax.broadcasted_iota(jnp.int32, (1, 2 * chunk), 1)
            limit = ((first_row + lax.rem(column, chunk)) // SPAN + 1) * SPAN
            key = lax.broadcasted_iota(jnp.int32, (tok_rows, 2 * chunk), 0)
            scores = jnp.where(key < limit, scores, NEG_FILL)
        old = top[n, 0:1]
        new = jnp.maximum(old, jnp.max(scores, axis=0, keepdims=True))
        expo = jnp.exp(scores - new).astype(jnp.bfloat16)
        acc[n] = acc[n] * jnp.exp(old - new) + jnp.dot(vals, expo, preferred_element_type=jnp.float32)
        top[n, 0:1] = new

    def own_shard(zz):
        return jnp.logical_and(zz == z, is_primary)

    def side(direct, lap):
        above = (odd == 1) if direct else (odd == 0)
        return lax.rem(region + jnp.where(above, lap, n_reg - lap), n_reg), above

    def shard_at(direct, k):
        lap, second = (k + 1) // 2, lax.rem(k + 1, 2)
        reg, above = side(direct, lap)
        far = jnp.where(k == n_reg - 1, 0, second)
        own = 2 * region + (odd if direct else 1 - odd)
        return jnp.where(k == 0, own, 2 * reg + jnp.where(above, far, 1 - far))

    def region_at(i):
        lap = (i + 1) // 2
        return jnp.where(lax.rem(i, 2) == 1, side(True, lap)[0], side(False, lap)[0])

    def use(p, c):
        reg, n = region_at(p // n_chunks), lax.rem(p, n_chunks)

        @pl.when(n > reg)
        def _():
            block(n, 2 * reg, None)
            block(n, 2 * reg + 1, None)

        @pl.when(n == reg)
        def _():
            last = lax.rem(chunk_of(n) // 2, 2)

            @pl.when(last == 1)
            def _():
                block(n, 2 * reg, None)

            block(n, 2 * reg + last, lax.rem(chunk_of(n), 2) * chunk)

        return c

    def take(zz, direct):
        @pl.when(jnp.logical_not(own_shard(zz)))
        def _():
            got(kvbuf.at[zz], kv_sem.at[zz])

            @pl.when(is_primary)
            def _():
                if direct:
                    remote(
                        kvbuf.at[zz], kvbuf.at[zz], fwd_chip.at[zz], kv_sem.at[zz], z + 1 - 2 * odd, core
                    ).start()
                remote(kvbuf.at[zz], kvbuf.at[zz], fwd_core.at[zz], kv_sem.at[zz], z, 1 - core).start()

    def arrive(i, used):
        @pl.when(i < n_reg)
        def _():
            take(shard_at(True, i), True)

        @pl.when(i == LEAD)
        def _():
            lax.fori_loop(0, n_chunks, ready, 0)

        def spend(used, done):
            whole = jnp.where(done < 1, 0, jnp.where(done == n_reg, n_reg, 2 * ((done - 1) // 2) + 2))
            whole = jnp.where(done == n_reg - 1, n_reg - 1, whole)
            upto = jnp.maximum(jnp.minimum(whole * n_chunks, used + QUOTA), used)
            lax.fori_loop(used, upto, use, 0)
            return upto

        used = spend(used, i - LEAD)

        @pl.when(i >= LEAD)
        def _():
            take(shard_at(False, i - LEAD), False)

        return spend(used, i - LEAD + 1)

    used = lax.fori_loop(0, n_reg + LEAD, arrive, jnp.int32(0))

    lam_rows = jnp.where(is_primary, lam_ref[...], lam_buf[...])
    lam_row = lam_rows[0:1]
    for head in range(1, heads_here):
        lam_row = jnp.where(home_head == head, lam_rows[head : head + 1], lam_row)
    gain = gain_ref[...]

    def o_dst(pr, b):
        head, seq = pr // seqs, lax.rem(pr, seqs)
        return nbuf.at[pl.ds(b * n_x // 2, n_x // 2), :, seq, :, pl.ds(pl.multiple_of(head * vdim, vdim), vdim)]

    def finish(n, carry):
        t = chunk_of(n)
        first, second = acc[n, :, :chunk], acc[n, :, chunk:]
        attn = first[:vdim] / first[vdim : vdim + 1] - lam_row[:, :1] * second[:vdim] / second[vdim : vdim + 1]
        mean_sq = jnp.mean(attn * attn, axis=0, keepdims=True)
        normed = ((attn * lax.rsqrt(mean_sq + EPS_NORM)).T * gain).astype(jnp.bfloat16)
        normed = normed.reshape(n_x // 2, 2, rows, vdim)
        b, zz = lax.rem(t, 2), t // 2
        here = local_chunk(n)
        ostage[n] = normed

        @pl.when(here)
        def _():
            o_dst(pair, b)[...] = normed

        @pl.when(jnp.logical_not(here))
        def _():
            remote(ostage.at[n], o_dst(pair, b), o_send.at[n], o_sem.at[2 * pair + b], zz, source_core).start()

        return carry

    def rest(n, carry):
        def visit(i, c):
            @pl.when(i * n_chunks + n >= used)
            def _():
                use(i * n_chunks + n, 0)

            return c

        lax.fori_loop(0, n_reg, visit, 0)
        return finish(n, carry)

    lax.fori_loop(0, n_chunks, rest, 0)

    def partial(cc, s):
        block = nbuf[:, cc, s].reshape(n_x * rows, heads_here * vdim)
        done = jnp.dot(block, wo_ref[...], preferred_element_type=jnp.float32)
        return done.astype(jnp.bfloat16).reshape(n_x, rows, width)

    def sib_copy(s):
        return remote(sib_out.at[s], sib_in.at[s], sib_send.at[s], sib_recv.at[s], z, 1 - core)

    def both(s, ahead, part):
        to_x = lax.rem(x + ahead + n_x, n_x)
        return mine[s, to_x, part].astype(jnp.float32) + sib_in[s, to_x, part].astype(jnp.float32)

    ways = (1, -1, 1, -1, 1, -1)

    def x_copy(s, i):
        at = len(ways) * s + i
        return to(xs.at[at], xr.at[at], x_send.at[at], x_recv.at[at], z, tp_of(ways[i], core))

    def ship(s, i, value):
        xs[len(ways) * s + i] = value.astype(jnp.bfloat16)
        x_copy(s, i).start()

    def came(s, i):
        at = len(ways) * s + i
        got(xr.at[at], x_recv.at[at])
        return xr[at].astype(jnp.float32)

    def sum_start(s):
        for k in range(s, n_pairs, seqs):
            for b in range(2):
                here, _, _ = q_copy(k, b)

                @pl.when(jnp.logical_not(here))
                def _():
                    got(o_dst(jnp.int32(k), b), o_sem.at[2 * k + b])

        sib_out[s] = partial(1 - core, s)
        sib_copy(s).start()
        mine[s] = partial(core, s)
        got(sib_in.at[s], sib_recv.at[s])
        ship(s, 0, both(s, 2, low))
        ship(s, 1, both(s, 2, high))
        ship(s, 2, both(s, 1, high))
        ship(s, 3, both(s, -1, low))

    def sum_pass(s):
        ship(s, 4, both(s, 1, low) + came(s, 0))
        ship(s, 5, both(s, -1, high) + came(s, 1))

    def sum_end(s):
        out_ref[s, low] = (both(s, 0, low) + came(s, 3) + came(s, 4)).astype(jnp.bfloat16)
        out_ref[s, high] = (both(s, 0, high) + came(s, 2) + came(s, 5)).astype(jnp.bfloat16)

    sum_start(0)
    sum_pass(0)
    sum_start(1)
    sum_end(0)
    sum_pass(1)
    sum_end(1)

    for s in range(seqs):
        sib_copy(s).wait_send()
        for i in range(len(ways)):
            x_copy(s, i).wait_send()
    for s in range(seqs):
        for copy in gather_copies(s):
            copy().wait_send()
    for k in range(n_pairs):
        here, copy = kv_copy(k)

        @pl.when(jnp.logical_not(here))
        def _():
            copy().wait_send()

        for b in range(2):
            q_here, _, q_sent = q_copy(k, b)

            @pl.when(jnp.logical_not(q_here))
            def _():
                q_sent().wait_send()

    def drain(n, carry):
        @pl.when(jnp.logical_not(local_chunk(n)))
        def _():
            remote(ostage.at[n], ostage.at[n], o_send.at[n], q_sem.at[n], z, 1 - core).wait_send()

        return carry

    lax.fori_loop(0, n_chunks, drain, 0)

    @pl.when(is_primary)
    def _():
        def sent(zz, carry):
            @pl.when(entry_of(region, zz) == z)
            def _():
                remote(kvbuf.at[zz], kvbuf.at[zz], fwd_chip.at[zz], kv_sem.at[zz], z, 1 - core).wait_send()

            remote(kvbuf.at[zz], kvbuf.at[zz], fwd_core.at[zz], kv_sem.at[zz], z, 1 - core).wait_send()
            return carry

        lax.fori_loop(0, n_sp, sent, 0)


def on_device(n_sp, n_tp, tokens, w_query, w_key, w_value, w_out, head_lambda, sub_gain):
    rows, seqs, width = tokens.shape
    heads_here = head_lambda.shape[0]
    vdim = sub_gain.shape[0]
    half = n_tp // 2
    chunk = half * rows
    n_pairs = seqs * heads_here
    n_chunks = n_sp // 2
    lam = jnp.broadcast_to(jnp.pad(head_lambda, (0, 8 - heads_here))[:, None], (8, vdim))
    turned = jnp.transpose(tokens, (1, 0, 2))
    dma = pltpu.SemaphoreType.DMA
    bf16, f32 = jnp.bfloat16, jnp.float32
    in_vmem = pl.BlockSpec(memory_space=pltpu.VMEM)
    out = pl.pallas_call(
        functools.partial(layer_kernel, n_sp),
        name="layer",
        out_shape=jax.ShapeDtypeStruct((seqs, rows, width), bf16),
        in_specs=[pl.BlockSpec(memory_space=pltpu.HBM)] + [in_vmem] * 6,
        out_specs=in_vmem,
        scratch_shapes=[
            pltpu.VMEM((seqs, n_tp, rows, width), bf16),
            pltpu.VMEM((n_pairs, 2 * chunk, vdim), bf16),
            pltpu.VMEM((n_pairs, 2, 2 * chunk, vdim), bf16),
            pltpu.VMEM((n_chunks, chunk, vdim), bf16),
            pltpu.VMEM((n_sp, 2, 2 * chunk, vdim), bf16),
            pltpu.VMEM((n_chunks, n_tp // 4, 2, rows, vdim), bf16),
            pltpu.VMEM((n_tp // 2, 2, seqs, rows, heads_here * vdim), bf16),
            pltpu.VMEM((8, vdim), f32),
            pltpu.VMEM((n_chunks, vdim, 2 * chunk), bf16),
            pltpu.VMEM((n_chunks, 8, 2 * chunk), f32),
            pltpu.VMEM((n_chunks, vdim + 16, 2 * chunk), f32),
            pltpu.VMEM((seqs, n_tp // 2, rows, width), bf16),
            pltpu.VMEM((seqs, n_tp // 2, rows, width), bf16),
            pltpu.VMEM((seqs, n_tp // 2, rows, width), bf16),
            pltpu.VMEM((6 * seqs, rows // 2, width), bf16),
            pltpu.VMEM((6 * seqs, rows // 2, width), bf16),
            dma((seqs * n_tp,)),
            dma((2 * seqs,)),
            dma((8 * seqs,)),
            dma((n_sp,)),
            dma((n_chunks,)),
            dma((2 * n_pairs,)),
            dma((n_pairs,)),
            dma((2 * n_pairs,)),
            dma((n_chunks,)),
            dma((n_sp,)),
            dma((n_sp,)),
            dma((2,)),
            dma((seqs,)),
            dma((seqs,)),
            dma((6 * seqs,)),
            dma((6 * seqs,)),
        ],
        compiler_params=pltpu.CompilerParams(
            collective_id=0, has_side_effects=True, vmem_limit_bytes=60 * 1024 * 1024
        ),
    )(turned, w_query, w_key, w_value, w_out, lam, sub_gain[None, :])
    return jnp.transpose(out, (1, 0, 2))


def solution(mesh):
    return jax.shard_map(
        functools.partial(on_device, mesh.shape["sp"], mesh.shape["tp"]),
        mesh=mesh,
        in_specs=(
            P(("grp", "sp", "tp"), None, None),
            P(None, "tp"),
            P(None, "tp"),
            P(None, "tp"),
            P("tp", None),
            P("tp"),
            P(),
        ),
        out_specs=P(("grp", "sp", "tp"), None, None),
        check_vma=False,
    )
```

```python
import functools

import jax
import jax.numpy as jnp
from jax import lax
from jax.experimental import pallas as pl
from jax.experimental.pallas import tpu as pltpu
from jax.sharding import PartitionSpec as P

SPAN = 64
NEG_FILL = -1e30
EPS_NORM = 1e-06
LEAD = 2
QUOTA = 2
MESH = pl.DeviceIdType.MESH


def layer_kernel(
    n_sp,
    turned,
    wq_ref,
    wk_ref,
    wv_ref,
    wo_ref,
    lam_ref,
    gain_ref,
    out_ref,
    tok,
    qj,
    kvj,
    qbuf,
    kvbuf,
    ostage,
    nbuf,
    lam_buf,
    qpad,
    top,
    acc,
    mine,
    sib_out,
    sib_in,
    xs,
    xr,
    ag_recv,
    ag_half,
    ag_send,
    kv_sem,
    q_sem,
    o_sem,
    kv_send,
    q_send,
    o_send,
    fwd_core,
    fwd_chip,
    lam_sem,
    sib_send,
    sib_recv,
    x_send,
    x_recv,
):
    seqs, groups, rows, width = tok.shape
    vdim = gain_ref.shape[1]
    head_dim = vdim // 2
    heads_here = wq_ref.shape[1] // vdim
    n_pairs = seqs * heads_here
    n_reg = n_sp // 2
    n_x = groups // 2
    half = groups // 2
    chunk = half * rows
    tok_rows = groups * rows
    n_chunks = n_sp // 2

    z = lax.axis_index("sp")
    tp = lax.axis_index("tp")
    core = lax.rem(tp, 2)
    x = tp // 2
    region = z // 2
    odd = lax.rem(z, 2)
    source_core = lax.rem(region, 2)
    is_primary = core == source_core
    pair = region // 2
    home_head, home_seq = pair // seqs, lax.rem(pair, seqs)
    rank = odd * 2 + core

    def tp_of(ahead, cc):
        return 2 * lax.rem(x + ahead + n_x, n_x) + cc

    def to(src, dst, send, recv, zz, tt):
        return pltpu.make_async_remote_copy(
            src_ref=src,
            dst_ref=dst,
            send_sem=send,
            recv_sem=recv,
            device_id={"sp": zz, "tp": tt},
            device_id_type=MESH,
        )

    def remote(src, dst, send, recv, zz, cc):
        return to(src, dst, send, recv, zz, 2 * x + cc)

    def got(ref, sem):
        pltpu.make_async_copy(ref, ref, sem).wait()

    def entry_of(reg, zz):
        ahead = lax.rem(reg - zz // 2 + n_reg, n_reg)
        up = jnp.logical_or(ahead < n_reg // 2, jnp.logical_and(ahead == n_reg // 2, lax.rem(zz, 2) == 1))
        return jnp.where(ahead == 0, zz, jnp.where(up, 2 * reg, 2 * reg + 1))

    barrier = pltpu.get_barrier_semaphore()

    def greet(i, carry):
        zz, cc = i // 2, lax.rem(i, 2)

        @pl.when(jnp.logical_or(zz != z, cc != core))
        def _():
            pl.semaphore_signal(barrier, inc=1, device_id={"sp": zz, "tp": 2 * x + cc}, device_id_type=MESH)

        return carry

    for ahead in (1, -1):
        pl.semaphore_signal(barrier, inc=1, device_id={"sp": z, "tp": tp_of(ahead, core)}, device_id_type=MESH)
    lax.fori_loop(0, 2 * n_sp, greet, 0)
    pl.semaphore_wait(barrier, 2 * n_sp + 1)

    low, high = slice(0, rows // 2), slice(rows // 2, rows)

    def gather_copies(s):
        own, back, fore, far = tp, tp_of(-1, core), tp_of(1, core), tp_of(2, core)

        def send(i, src, dst, sem, tt):
            return to(src, dst, ag_send.at[10 * s + i], sem, z, tt)

        sib = 2 * x + 1 - core

        def full(i, t, tt):
            return send(i, tok.at[s, t], tok.at[s, t], ag_recv.at[groups * s + t], tt)

        return (
            lambda: send(0, turned.at[s, low], tok.at[s, own, low], ag_half.at[6 * s + 2], fore),
            lambda: send(1, turned.at[s, high], tok.at[s, own, high], ag_half.at[6 * s + 4], back),
            lambda: send(2, turned.at[s], tok.at[s, own], ag_recv.at[groups * s + own], sib),
            lambda: send(3, tok.at[s, back, low], tok.at[s, back, low], ag_half.at[6 * s], fore),
            lambda: send(4, tok.at[s, fore, high], tok.at[s, fore, high], ag_half.at[6 * s + 1], back),
            lambda: full(5, back, sib),
            lambda: full(6, fore, sib),
            lambda: full(7, far, sib),
            lambda: send(8, turned.at[s, high], tok.at[s, own, high], ag_half.at[6 * s + 3], fore),
            lambda: send(9, turned.at[s, low], tok.at[s, own, low], ag_half.at[6 * s + 5], back),
        )

    def gather_start(s):
        pltpu.make_async_copy(turned.at[s], tok.at[s, tp], ag_recv.at[groups * s + tp]).start()
        copies = gather_copies(s)
        for i in (0, 1, 8, 9, 2):
            copies[i]().start()

    def gather_near(s):
        copies = gather_copies(s)
        back, fore = tp_of(-1, core), tp_of(1, core)
        got(tok.at[s, back, low], ag_half.at[6 * s + 2])
        copies[3]().start()
        got(tok.at[s, fore, high], ag_half.at[6 * s + 4])
        copies[4]().start()
        got(tok.at[s, back, high], ag_half.at[6 * s + 3])
        copies[5]().start()
        got(tok.at[s, fore, low], ag_half.at[6 * s + 5])
        copies[6]().start()

    def gather_far(s):
        t = tp_of(2, core)
        got(tok.at[s, t, low], ag_half.at[6 * s])
        got(tok.at[s, t, high], ag_half.at[6 * s + 1])
        gather_copies(s)[7]().start()
        got(tok.at[s, tp], ag_recv.at[groups * s + tp])
        for ahead in (0, 1, -1, 2):
            t = tp_of(ahead, 1 - core)
            got(tok.at[s, t], ag_recv.at[groups * s + t])

    def project(s):
        def tile(i, carry):
            block = tok[s, pl.ds(i * half, half)].reshape(chunk, width)
            at = pl.ds(pl.multiple_of(i * chunk, chunk), chunk)
            keys = jnp.dot(block, wk_ref[...], preferred_element_type=jnp.float32).astype(jnp.bfloat16)
            vals = jnp.dot(block, wv_ref[...], preferred_element_type=jnp.float32).T.astype(jnp.bfloat16)
            queries = jnp.dot(block, wq_ref[...], preferred_element_type=jnp.float32).astype(jnp.bfloat16)
            for head in range(heads_here):
                k, cut = head * seqs + s, slice(head * vdim, (head + 1) * vdim)
                qj[k, at] = queries[:, cut]
                kvj[k, 0, at] = keys[:, cut]
                for part in range(chunk // vdim):
                    first = pl.multiple_of(i * chunk + part * vdim, vdim)
                    kvj[k, 1, pl.ds(first, vdim)] = vals[cut, part * vdim : (part + 1) * vdim]
            return carry

        lax.fori_loop(0, 2, tile, 0)

    def kv_src(k):
        return kvj.at[k]

    def q_src(k, b):
        return qj.at[k, b * chunk : (b + 1) * chunk]

    def q_place(b):
        t = 2 * z + b
        u = lax.rem(t, 8)
        rk = jnp.where(u < 4, u, 7 - u)
        return rk // 2, lax.rem(rk, 2), (t // 8) * 2 + u // 4

    def q_copy(k, b):
        rz, rc, slot = q_place(b)
        zz = 2 * (2 * k + core) + rz
        here = jnp.logical_and(zz == z, rc == core)
        return here, slot, lambda: remote(q_src(k, b), qbuf.at[slot], q_send.at[2 * k + b], q_sem.at[slot], zz, rc)

    def kv_copy(k):
        ent = entry_of(2 * k + core, z)
        return ent == z, lambda: remote(kv_src(k), kvbuf.at[z], kv_send.at[k], kv_sem.at[z], ent, core)

    def send_queries(s):
        for k in range(s, n_pairs, seqs):
            for b in range(2):
                here, slot, copy = q_copy(k, b)

                @pl.when(here)
                def _():
                    qbuf[slot] = q_src(k, b)[...]

                @pl.when(jnp.logical_not(here))
                def _():
                    copy().start()

    def send_keys():
        for k in range(n_pairs):
            here, _ = kv_copy(k)

            @pl.when(here)
            def _():
                remote(kv_src(k), kvbuf.at[z], fwd_chip.at[z], kv_sem.at[z], z + 1 - 2 * odd, core).start()
                remote(kv_src(k), kvbuf.at[z], fwd_core.at[z], kv_sem.at[z], z, 1 - core).start()
                kvbuf[z] = kv_src(k)[...]

        for near in (True, False):
            for k in range(n_pairs):
                here, copy = kv_copy(k)
                ahead = lax.rem(2 * k + core - region + n_reg, n_reg)
                close = jnp.minimum(ahead, n_reg - ahead) <= n_reg // 4

                @pl.when(jnp.logical_and(jnp.logical_not(here), close if near else jnp.logical_not(close)))
                def _():
                    copy().start()

    lam_copy = remote(lam_ref, lam_buf, lam_sem.at[0], lam_sem.at[1], z, 1 - core)
    lam_copy.start()
    gather_start(0)
    gather_near(0)
    gather_start(1)
    gather_far(0)
    project(0)
    send_queries(0)
    gather_near(1)
    gather_far(1)
    project(1)
    send_queries(1)
    send_keys()
    lam_copy.wait()

    channel = lax.broadcasted_iota(jnp.int32, (vdim, chunk), 0)
    ones = jnp.ones((acc.shape[1] - vdim, tok_rows), jnp.bfloat16)

    def chunk_of(n):
        return (n // 2) * 8 + jnp.where(lax.rem(n, 2) == 1, 7 - rank, rank)

    def local_chunk(n):
        t = chunk_of(n)
        return jnp.logical_and(t // 2 == z, is_primary)

    def ready(n, carry):
        @pl.when(jnp.logical_not(local_chunk(n)))
        def _():
            got(qbuf.at[n], q_sem.at[n])

        query = qbuf[n].astype(jnp.float32).T * head_dim ** (-0.5)
        qpad[n, :, :chunk] = jnp.where(channel < head_dim, query, 0.0).astype(jnp.bfloat16)
        qpad[n, :, chunk:] = jnp.where(channel < head_dim, 0.0, query).astype(jnp.bfloat16)
        top[n] = jnp.full(top.shape[1:], NEG_FILL, jnp.float32)
        acc[n] = jnp.zeros(acc.shape[1:], jnp.float32)
        return carry

    def block(n, zz, first_row):
        turned_vals = kvbuf[zz, 1].reshape(tok_rows // vdim, vdim, vdim)
        vals = jnp.concatenate([turned_vals[i] for i in range(tok_rows // vdim)], axis=1)
        vals = jnp.concatenate([vals, ones], axis=0)
        scores = jnp.dot(kvbuf[zz, 0], qpad[n], preferred_element_type=jnp.float32)
        if first_row is not None:
            column = lax.broadcasted_iota(jnp.int32, (1, 2 * chunk), 1)
            limit = ((first_row + lax.rem(column, chunk)) // SPAN + 1) * SPAN
            key = lax.broadcasted_iota(jnp.int32, (tok_rows, 2 * chunk), 0)
            scores = jnp.where(key < limit, scores, NEG_FILL)
        old = top[n, 0:1]
        new = jnp.maximum(old, jnp.max(scores, axis=0, keepdims=True))
        expo = jnp.exp(scores - new).astype(jnp.bfloat16)
        acc[n] = acc[n] * jnp.exp(old - new) + jnp.dot(vals, expo, preferred_element_type=jnp.float32)
        top[n, 0:1] = new

    def own_shard(zz):
        return jnp.logical_and(zz == z, is_primary)

    def side(direct, lap):
        above = (odd == 1) if direct else (odd == 0)
        return lax.rem(region + jnp.where(above, lap, n_reg - lap), n_reg), above

    def shard_at(direct, k):
        lap, second = (k + 1) // 2, lax.rem(k + 1, 2)
        reg, above = side(direct, lap)
        far = jnp.where(k == n_reg - 1, 0, second)
        own = 2 * region + (odd if direct else 1 - odd)
        return jnp.where(k == 0, own, 2 * reg + jnp.where(above, far, 1 - far))

    def region_at(i):
        lap = (i + 1) // 2
        return jnp.where(lax.rem(i, 2) == 1, side(True, lap)[0], side(False, lap)[0])

    def use(p, c):
        reg, n = region_at(p // n_chunks), lax.rem(p, n_chunks)

        @pl.when(n > reg)
        def _():
            block(n, 2 * reg, None)
            block(n, 2 * reg + 1, None)

        @pl.when(n == reg)
        def _():
            last = lax.rem(chunk_of(n) // 2, 2)

            @pl.when(last == 1)
            def _():
                block(n, 2 * reg, None)

            block(n, 2 * reg + last, lax.rem(chunk_of(n), 2) * chunk)

        return c

    def take(zz, direct):
        @pl.when(jnp.logical_not(own_shard(zz)))
        def _():
            got(kvbuf.at[zz], kv_sem.at[zz])

            @pl.when(is_primary)
            def _():
                if direct:
                    remote(
                        kvbuf.at[zz], kvbuf.at[zz], fwd_chip.at[zz], kv_sem.at[zz], z + 1 - 2 * odd, core
                    ).start()
                remote(kvbuf.at[zz], kvbuf.at[zz], fwd_core.at[zz], kv_sem.at[zz], z, 1 - core).start()

    def arrive(i, used):
        @pl.when(i < n_reg)
        def _():
            take(shard_at(True, i), True)

        @pl.when(i == LEAD)
        def _():
            lax.fori_loop(0, n_chunks, ready, 0)

        def spend(used, done):
            whole = jnp.where(done < 1, 0, jnp.where(done == n_reg, n_reg, 2 * ((done - 1) // 2) + 2))
            whole = jnp.where(done == n_reg - 1, n_reg - 1, whole)
            upto = jnp.maximum(jnp.minimum(whole * n_chunks, used + QUOTA), used)
            lax.fori_loop(used, upto, use, 0)
            return upto

        used = spend(used, i - LEAD)

        @pl.when(i >= LEAD)
        def _():
            take(shard_at(False, i - LEAD), False)

        return spend(used, i - LEAD + 1)

    used = lax.fori_loop(0, n_reg + LEAD, arrive, jnp.int32(0))

    lam_rows = jnp.where(is_primary, lam_ref[...], lam_buf[...])
    lam_row = lam_rows[0:1]
    for head in range(1, heads_here):
        lam_row = jnp.where(home_head == head, lam_rows[head : head + 1], lam_row)
    gain = gain_ref[...]

    def o_dst(pr, b):
        head, seq = pr // seqs, lax.rem(pr, seqs)
        return nbuf.at[pl.ds(b * n_x // 2, n_x // 2), :, seq, :, pl.ds(pl.multiple_of(head * vdim, vdim), vdim)]

    def finish(n, carry):
        t = chunk_of(n)
        first, second = acc[n, :, :chunk], acc[n, :, chunk:]
        attn = first[:vdim] / first[vdim : vdim + 1] - lam_row[:, :1] * second[:vdim] / second[vdim : vdim + 1]
        mean_sq = jnp.mean(attn * attn, axis=0, keepdims=True)
        normed = ((attn * lax.rsqrt(mean_sq + EPS_NORM)).T * gain).astype(jnp.bfloat16)
        normed = normed.reshape(n_x // 2, 2, rows, vdim)
        b, zz = lax.rem(t, 2), t // 2
        here = local_chunk(n)
        ostage[n] = normed

        @pl.when(here)
        def _():
            o_dst(pair, b)[...] = normed

        @pl.when(jnp.logical_not(here))
        def _():
            remote(ostage.at[n], o_dst(pair, b), o_send.at[n], o_sem.at[2 * pair + b], zz, source_core).start()

        return carry

    def rest(n, carry):
        def visit(i, c):
            @pl.when(i * n_chunks + n >= used)
            def _():
                use(i * n_chunks + n, 0)

            return c

        lax.fori_loop(0, n_reg, visit, 0)
        return finish(n, carry)

    lax.fori_loop(0, n_chunks, rest, 0)

    def partial(cc, s):
        block = nbuf[:, cc, s].reshape(n_x * rows, heads_here * vdim)
        done = jnp.dot(block, wo_ref[...], preferred_element_type=jnp.float32)
        return done.astype(jnp.bfloat16).reshape(n_x, rows, width)

    def sib_copy(s):
        return remote(sib_out.at[s], sib_in.at[s], sib_send.at[s], sib_recv.at[s], z, 1 - core)

    def both(s, ahead, part):
        to_x = lax.rem(x + ahead + n_x, n_x)
        return mine[s, to_x, part].astype(jnp.float32) + sib_in[s, to_x, part].astype(jnp.float32)

    ways = (1, -1, 1, -1, 1, -1)

    def x_copy(s, i):
        at = len(ways) * s + i
        return to(xs.at[at], xr.at[at], x_send.at[at], x_recv.at[at], z, tp_of(ways[i], core))

    def ship(s, i, value):
        xs[len(ways) * s + i] = value.astype(jnp.bfloat16)
        x_copy(s, i).start()

    def came(s, i):
        at = len(ways) * s + i
        got(xr.at[at], x_recv.at[at])
        return xr[at].astype(jnp.float32)

    def sum_start(s):
        for k in range(s, n_pairs, seqs):
            for b in range(2):
                here, _, _ = q_copy(k, b)

                @pl.when(jnp.logical_not(here))
                def _():
                    got(o_dst(jnp.int32(k), b), o_sem.at[2 * k + b])

        sib_out[s] = partial(1 - core, s)
        sib_copy(s).start()
        mine[s] = partial(core, s)
        got(sib_in.at[s], sib_recv.at[s])
        ship(s, 0, both(s, 2, low))
        ship(s, 1, both(s, 2, high))
        ship(s, 2, both(s, 1, high))
        ship(s, 3, both(s, -1, low))

    def sum_pass(s):
        ship(s, 4, both(s, 1, low) + came(s, 0))
        ship(s, 5, both(s, -1, high) + came(s, 1))

    def sum_end(s):
        out_ref[s, low] = (both(s, 0, low) + came(s, 3) + came(s, 4)).astype(jnp.bfloat16)
        out_ref[s, high] = (both(s, 0, high) + came(s, 2) + came(s, 5)).astype(jnp.bfloat16)

    sum_start(0)
    sum_pass(0)
    sum_start(1)
    sum_end(0)
    sum_pass(1)
    sum_end(1)

    for s in range(seqs):
        sib_copy(s).wait_send()
        for i in range(len(ways)):
            x_copy(s, i).wait_send()
    for s in range(seqs):
        for copy in gather_copies(s):
            copy().wait_send()
    for k in range(n_pairs):
        here, copy = kv_copy(k)

        @pl.when(jnp.logical_not(here))
        def _():
            copy().wait_send()

        for b in range(2):
            q_here, _, q_sent = q_copy(k, b)

            @pl.when(jnp.logical_not(q_here))
            def _():
                q_sent().wait_send()

    def drain(n, carry):
        @pl.when(jnp.logical_not(local_chunk(n)))
        def _():
            remote(ostage.at[n], ostage.at[n], o_send.at[n], q_sem.at[n], z, 1 - core).wait_send()

        return carry

    lax.fori_loop(0, n_chunks, drain, 0)

    @pl.when(is_primary)
    def _():
        def sent(zz, carry):
            @pl.when(entry_of(region, zz) == z)
            def _():
                remote(kvbuf.at[zz], kvbuf.at[zz], fwd_chip.at[zz], kv_sem.at[zz], z, 1 - core).wait_send()

            remote(kvbuf.at[zz], kvbuf.at[zz], fwd_core.at[zz], kv_sem.at[zz], z, 1 - core).wait_send()
            return carry

        lax.fori_loop(0, n_sp, sent, 0)


def on_device(n_sp, n_tp, tokens, w_query, w_key, w_value, w_out, head_lambda, sub_gain):
    rows, seqs, width = tokens.shape
    heads_here = head_lambda.shape[0]
    vdim = sub_gain.shape[0]
    half = n_tp // 2
    chunk = half * rows
    n_pairs = seqs * heads_here
    n_chunks = n_sp // 2
    lam = jnp.broadcast_to(jnp.pad(head_lambda, (0, 8 - heads_here))[:, None], (8, vdim))
    turned = jnp.transpose(tokens, (1, 0, 2))
    dma = pltpu.SemaphoreType.DMA
    bf16, f32 = jnp.bfloat16, jnp.float32
    in_vmem = pl.BlockSpec(memory_space=pltpu.VMEM)
    out = pl.pallas_call(
        functools.partial(layer_kernel, n_sp),
        name="layer",
        out_shape=jax.ShapeDtypeStruct((seqs, rows, width), bf16),
        in_specs=[pl.BlockSpec(memory_space=pltpu.HBM)] + [in_vmem] * 6,
        out_specs=in_vmem,
        scratch_shapes=[
            pltpu.VMEM((seqs, n_tp, rows, width), bf16),
            pltpu.VMEM((n_pairs, 2 * chunk, vdim), bf16),
            pltpu.VMEM((n_pairs, 2, 2 * chunk, vdim), bf16),
            pltpu.VMEM((n_chunks, chunk, vdim), bf16),
            pltpu.VMEM((n_sp, 2, 2 * chunk, vdim), bf16),
            pltpu.VMEM((n_chunks, n_tp // 4, 2, rows, vdim), bf16),
            pltpu.VMEM((n_tp // 2, 2, seqs, rows, heads_here * vdim), bf16),
            pltpu.VMEM((8, vdim), f32),
            pltpu.VMEM((n_chunks, vdim, 2 * chunk), bf16),
            pltpu.VMEM((n_chunks, 8, 2 * chunk), f32),
            pltpu.VMEM((n_chunks, vdim + 16, 2 * chunk), f32),
            pltpu.VMEM((seqs, n_tp // 2, rows, width), bf16),
            pltpu.VMEM((seqs, n_tp // 2, rows, width), bf16),
            pltpu.VMEM((seqs, n_tp // 2, rows, width), bf16),
            pltpu.VMEM((6 * seqs, rows // 2, width), bf16),
            pltpu.VMEM((6 * seqs, rows // 2, width), bf16),
            dma((seqs * n_tp,)),
            dma((6 * seqs,)),
            dma((10 * seqs,)),
            dma((n_sp,)),
            dma((n_chunks,)),
            dma((2 * n_pairs,)),
            dma((n_pairs,)),
            dma((2 * n_pairs,)),
            dma((n_chunks,)),
            dma((n_sp,)),
            dma((n_sp,)),
            dma((2,)),
            dma((seqs,)),
            dma((seqs,)),
            dma((6 * seqs,)),
            dma((6 * seqs,)),
        ],
        compiler_params=pltpu.CompilerParams(
            collective_id=0, has_side_effects=True, vmem_limit_bytes=60 * 1024 * 1024
        ),
    )(turned, w_query, w_key, w_value, w_out, lam, sub_gain[None, :])
    return jnp.transpose(out, (1, 0, 2))


def solution(mesh):
    return jax.shard_map(
        functools.partial(on_device, mesh.shape["sp"], mesh.shape["tp"]),
        mesh=mesh,
        in_specs=(
            P(("grp", "sp", "tp"), None, None),
            P(None, "tp"),
            P(None, "tp"),
            P(None, "tp"),
            P("tp", None),
            P("tp"),
            P(),
        ),
        out_specs=P(("grp", "sp", "tp"), None, None),
        check_vma=False,
    )
```
